32 devices in a mesh: sp: 16 (over z, y, x), tp: 2 (over core).
Axes of the slice: x: 2, y: 2, z: 4, core: 2. Of those that a mesh axis runs over, the one named last changes fastest.
Arguments:
- resid: bfloat16 [8192, 2048], P('sp'), may hold values from -6 to 6
- queries: bfloat16 [8192, 2048], P('sp', 'tp'), may hold values from -6 to 6
- keys: bfloat16 [8192, 512], P('sp', 'tp'), may hold values from -6 to 6
- values: bfloat16 [8192, 512], P('sp', 'tp'), may hold values from -6 to 6
- documents: int32 [8192], P('sp'), may hold values from 0 to 7, never falling along the last dimension, each value on 1 to 2048 neighbouring positions
- q_gain: float32 [64], replicated, may hold values from 0.5 to 6.5
- k_gain: float32 [64], replicated, may hold values from 0.5 to 6.5
- sink: float32 [32], P('tp'), may hold values from -1 to 5
- w_out: bfloat16 [2048, 2048], P('tp'), may hold values from -0.5 to 0.5
- n_gain: float32 [2048], replicated, may hold values from 0.1 to 1.9
- w_up: bfloat16 [2048, 8192], P('sp', 'tp'), may hold values from -0.125 to 0.125
- w_down: bfloat16 [8192, 2048], P('tp', 'sp'), may hold values from -0.0625 to 0.0625
Outputs:
- layer_out: bfloat16 [8192, 2048], P('sp')
The draws below stay inside these ranges and needn't reach their ends.
All inputs are finite; a program needn't handle non-finite values.
Results may differ from the reference program's by a relative error of at most 0.018.
The reference program's roundings to bfloat16 on the way count: a program that leaves them out, or rounds other values in their place, can miss the bound.
Values may be sent and summed in bfloat16 or wider, within the bound.
A program may use at most 128 MiB of HBM per device.

```python
import math
import jax
import jax.numpy as jnp
import numpy as np
from jax import lax

D = 2048
HEADS = 32
KV_HEADS = 8
HEAD = 64
FF = 8192
WINDOW = 128
TOK_DEV = 512
TOKENS = 8192
N_SP = 16
N_TP = 2


def base_keys(key):
    return jax.random.normal(jax.random.fold_in(key, 3), (TOKENS, KV_HEADS * HEAD), jnp.float32)


def draw_keys(key, part):
    drawn = base_keys(key)
    return jnp.clip(drawn, -6.0, 6.0).astype(jnp.bfloat16)


def draw_queries(key, part):
    drawn = jax.random.normal(jax.random.fold_in(key, 7), (TOKENS, HEADS * HEAD), jnp.float32)
    return jnp.clip(drawn, -6.0, 6.0).astype(jnp.bfloat16)


def draw_q_gain(key, part):
    return jax.random.uniform(jax.random.fold_in(key, 21), (HEAD,), jnp.float32, 0.5, 1.5)


def draw_k_gain(key, part):
    return jax.random.uniform(jax.random.fold_in(key, 23), (HEAD,), jnp.float32, 0.5, 1.5)


def block_levels(key, shape, cuts, least, top_value):
    level, own = 1.0, jax.random.fold_in(key, 6)
    for position, shards_of in cuts:
        draws = jnp.exp(jax.random.uniform(jax.random.fold_in(own, position), (shards_of,), jnp.float32, least / len(cuts), top_value / len(cuts)))
        level = level * jnp.repeat(draws, shape[position] // shards_of).reshape([-1 if axis == position else 1 for axis in range(len(shape))])
    return level


def profile(number_of, total, bound, lean):
    loads = [(1 << 20) // math.isqrt(rank ** lean) + 1 for rank in range(2, number_of + 1)]
    rest, holding = total - bound - (number_of - 1), [1] * (number_of - 1)
    while rest > 0:
        candidates = [i for i in range(number_of - 1) if holding[i] < bound]
        mass, budget = sum([loads[i] for i in candidates]), rest
        for i in candidates:
            extra = min(bound - holding[i], max(1, budget * loads[i] // mass), rest)
            holding[i] = holding[i] + extra
            rest = rest - extra
    return np.array([bound] + holding)


def uneven(key, amount, total, limit, lean):
    if amount == 2:
        one = jax.random.randint(key, (), max(1, total - limit), min(limit, total - 1) + 1)
        return jnp.stack([one, total - one])
    sizes = jnp.asarray(profile(amount, total, limit, lean), jnp.int32)
    twos = (amount - 1) // 2
    source_of, taker = sizes[1:1 + 2 * twos:2], sizes[2:2 + 2 * twos:2]
    slack = jnp.minimum(source_of - 1, limit - taker)
    passed = jax.random.randint(jax.random.fold_in(key, 1), (twos,), 0, 1 << 20) % (slack + 1)
    sizes = sizes.at[1:1 + 2 * twos:2].set(source_of - passed).at[2:2 + 2 * twos:2].set(taker + passed)
    return sizes[jax.random.permutation(jax.random.fold_in(key, 2), amount)]


def gaussian(stream_key, extent, deviation, bound, cuts=(), kind=jnp.bfloat16):
    result = jax.random.normal(stream_key, extent, jnp.float32) * deviation
    if len(cuts) > 0:
        result = block_levels(stream_key, extent, cuts, -0.22, 0.18) * result
    return jnp.clip(result, min=-bound, max=bound).astype(kind)


def setup_inputs(seed: int = 0) -> dict:
    splits = jax.random.split(jax.random.key(seed), 13)
    resid = gaussian(splits[0], (TOKENS, D), 1.0, 6.0, ((0, 16),))
    queries = draw_queries(jax.random.fold_in(splits[12], 71), 0)
    keys = draw_keys(jax.random.fold_in(splits[12], 71), 0)
    values = gaussian(splits[3], (TOKENS, KV_HEADS * HEAD), 1.0, 6.0, ((0, 16), (1, 2)))
    documents = jnp.searchsorted(jnp.cumsum(uneven(splits[4], N_SP // 2, TOKENS, 4 * TOK_DEV, 0)), jnp.arange(TOKENS), side="right").astype(jnp.int32)
    q_gain = draw_q_gain(jax.random.fold_in(splits[12], 71), 0)
    k_gain = draw_k_gain(jax.random.fold_in(splits[12], 71), 0)
    sink = jnp.clip(-1.0 + 6.0 * jax.random.uniform(splits[7], (HEADS,), jnp.float32) ** block_levels(splits[7], (HEADS,), ((0, 2),), -0.2, 0.2), -1.0, 5.0)
    w_out = gaussian(splits[8], (HEADS * HEAD, D), (HEADS * HEAD // 16) ** -0.5, 0.5, ((0, 2),))
    n_gain = jnp.clip(1.0 + 0.18 * jax.random.normal(splits[9], (D,), jnp.float32), 0.1, 1.9)
    w_up = gaussian(splits[10], (D, FF), D ** -0.5, 0.125, ((0, 16), (1, 2)))
    w_down = gaussian(splits[11], (FF, D), FF ** -0.5, 0.0625, ((0, 2), (1, 16)))
    return dict(resid=resid, queries=queries, keys=keys, values=values, documents=documents, q_gain=q_gain, k_gain=k_gain, sink=sink, w_out=w_out, n_gain=n_gain, w_up=w_up, w_down=w_down)


EPS = 1e-06

def rms_scale(field, gain):
    wide = field.astype(jnp.float32)
    return wide * lax.rsqrt(lax.optimization_barrier(jnp.mean(wide * wide, axis=-1, keepdims=True)) + EPS) * gain.astype(jnp.float32)

def reference(resid, queries, keys, values, documents, q_gain, k_gain, sink, w_out, n_gain, w_up, w_down):
    group = HEADS // KV_HEADS
    qnorm = rms_scale(queries.reshape(TOKENS, KV_HEADS, group, HEAD), q_gain).astype(jnp.bfloat16)
    knorm = rms_scale(keys.reshape(TOKENS, KV_HEADS, HEAD), k_gain).astype(jnp.bfloat16)
    vheads = values.reshape(TOKENS, KV_HEADS, HEAD)
    padding = ((WINDOW, WINDOW), (0, 0), (0, 0))
    key_pad = jnp.pad(knorm, padding)
    value_pad = jnp.pad(vheads, padding)
    doc_pad = jnp.pad(documents, (WINDOW, WINDOW), constant_values=-1)
    slopes = jnp.exp2(-8.0 * (jnp.arange(HEADS, dtype=jnp.float32) + 1.0) / HEADS).reshape(KV_HEADS, group)
    sink_f = sink.astype(jnp.float32).reshape(KV_HEADS, group)
    span = TOK_DEV
    blocks = TOKENS // span
    query_blocks = qnorm.reshape(blocks, span, KV_HEADS, group, HEAD)
    doc_blocks = documents.reshape(blocks, span)

    def one_block(args):
        qblock, dblock, number = args
        start = number * span
        kblock = lax.dynamic_slice_in_dim(key_pad, start, span + 2 * WINDOW, 0)
        vblock = lax.dynamic_slice_in_dim(value_pad, start, span + 2 * WINDOW, 0)
        dkeys = lax.dynamic_slice_in_dim(doc_pad, start, span + 2 * WINDOW, 0)
        query_pos = start + jnp.arange(span, dtype=jnp.int32)
        key_pos = start - WINDOW + jnp.arange(span + 2 * WINDOW, dtype=jnp.int32)
        distance = key_pos[None, :] - query_pos[:, None]
        allowed = (jnp.abs(distance) <= WINDOW) & (key_pos[None, :] >= 0) & (key_pos[None, :] < TOKENS)
        allowed = allowed & (dkeys[None, :] == dblock[:, None])
        scores = jnp.einsum('rkgd,skd->kgrs', qblock.astype(jnp.float32), kblock.astype(jnp.float32)) * HEAD ** (-0.5)
        scores = scores - slopes[:, :, None, None] * jnp.abs(distance).astype(jnp.float32)[None, None]
        scores = jnp.where(allowed[None, None], scores, jnp.float32(-1e+30))
        highest = jnp.maximum(lax.optimization_barrier(jnp.max(scores, axis=-1)), sink_f[:, :, None])
        weights = jnp.exp(scores - highest[..., None])
        denom = lax.optimization_barrier(jnp.sum(weights, axis=-1)) + jnp.exp(sink_f[:, :, None] - highest)
        rounded = weights.astype(jnp.bfloat16)
        summed = jnp.einsum('kgrs,skd->rkgd', rounded.astype(jnp.float32), vblock.astype(jnp.float32))
        return (summed / denom.transpose(2, 0, 1)[..., None]).astype(jnp.bfloat16)
    attended = lax.map(one_block, (query_blocks, doc_blocks, jnp.arange(blocks, dtype=jnp.int32)))
    attended = attended.reshape(TOKENS, HEADS * HEAD)
    cols = HEADS * HEAD // N_TP
    head_mix = jnp.zeros((TOKENS, D), jnp.float32)
    for index in range(N_TP):
        partial_sum = jnp.dot(attended[:, index * cols:(index + 1) * cols], w_out[index * cols:(index + 1) * cols], preferred_element_type=jnp.float32)
        head_mix = head_mix + partial_sum.astype(jnp.bfloat16).astype(jnp.float32)
    middle = (resid.astype(jnp.float32) + head_mix).astype(jnp.bfloat16)
    normed = rms_scale(middle, n_gain).astype(jnp.bfloat16)
    units = FF // N_TP
    unit_mix = jnp.zeros((TOKENS, D), jnp.float32)
    for index in range(N_TP):
        upward = jnp.dot(normed, w_up[:, index * units:(index + 1) * units], preferred_element_type=jnp.float32)
        active = jnp.square(jax.nn.relu(upward)).astype(jnp.bfloat16)
        partial_sum = jnp.dot(active, w_down[index * units:(index + 1) * units], preferred_element_type=jnp.float32)
        unit_mix = unit_mix + partial_sum.astype(jnp.bfloat16).astype(jnp.float32)
    return (middle.astype(jnp.float32) + unit_mix).astype(jnp.bfloat16)
```

```python
import functools

import jax
import jax.numpy as jnp
from jax import lax
from jax.experimental import pallas as pl
from jax.experimental.pallas import tpu as pltpu
from jax.sharding import PartitionSpec as P

WINDOW = 128
EPS = 1e-06
MEMBERS = 4
F32 = jnp.float32
BF16 = jnp.bfloat16
MESH = pl.DeviceIdType.MESH


def rms(wide, gain):
    return wide * lax.rsqrt(jnp.mean(wide * wide, axis=-1, keepdims=True) + EPS) * gain


def kernel(
    n_sp,
    head,
    heads,
    kv_heads,
    resid,
    queries,
    keys,
    values,
    doc_col,
    doc_row,
    q_gain,
    k_gain,
    slopes,
    sink,
    w_out,
    n_gain,
    w_up,
    w_down,
    out,
    kx,
    vx,
    dx,
    kn,
    att,
    wo,
    res,
    mine,
    other,
    other_in,
    mid,
    normed,
    wu,
    wd,
    act,
    part,
    twin_out,
    twin_in,
    sum_out,
    sum_in,
    half_out,
    half_in,
    halo_send,
    halo_recv,
    w_send,
    w_recv,
    w_local,
    loc_sem,
    tok_send,
    tok_recv,
    pair_send,
    pair_recv,
    misc_send,
    misc_recv,
):
    rows = queries.shape[0]
    half = rows // 2
    depth = w_up.shape[0]
    units = wu.shape[1]
    width = wd.shape[1]
    group = heads // kv_heads
    n_za = n_sp // 8

    sp = lax.axis_index("sp")
    t = lax.axis_index("tp")
    u = 1 - t
    x = sp % 2
    y = (sp // 2) % 2
    zb = (sp // 4) % 2
    za = sp // 8
    me = zb * 2 + x

    def index(za_, zb_, y_, x_):
        return za_ * 8 + zb_ * 4 + y_ * 2 + x_

    def flip(v, by):
        return 1 - v if by else v

    def remote(src, dst, send, recv, where):
        return pltpu.make_async_remote_copy(
            src_ref=src, dst_ref=dst, send_sem=send, recv_sem=recv,
            device_id=where, device_id_type=MESH,
        )

    load_wo = pltpu.make_async_copy(w_out, wo, loc_sem.at[0])
    load_wo.start()
    load_res = pltpu.make_async_copy(resid.at[pl.ds(t * half, half), :], res, loc_sem.at[1])
    load_res.start()
    own_k = pltpu.make_async_copy(keys, kx.at[pl.ds(WINDOW, rows), :], loc_sem.at[2])
    own_v = pltpu.make_async_copy(values, vx.at[pl.ds(WINDOW, rows), :], loc_sem.at[3])
    own_d = pltpu.make_async_copy(doc_row, dx.at[:, pl.ds(WINDOW, rows)], loc_sem.at[4])
    own_k.start()
    own_v.start()
    own_d.start()

    def halo(side, where):
        src = rows - WINDOW if side == 0 else 0
        dst = 0 if side == 0 else WINDOW + rows
        return [
            remote(keys.at[pl.ds(src, WINDOW), :], kx.at[pl.ds(dst, WINDOW), :],
                   halo_send.at[side, 0], halo_recv.at[side, 0], where),
            remote(values.at[pl.ds(src, WINDOW), :], vx.at[pl.ds(dst, WINDOW), :],
                   halo_send.at[side, 1], halo_recv.at[side, 1], where),
            remote(doc_row.at[:, pl.ds(src, WINDOW)], dx.at[:, pl.ds(dst, WINDOW)],
                   halo_send.at[side, 2], halo_recv.at[side, 2], where),
        ]

    up_to = lax.rem(sp + 1, n_sp)
    down_to = lax.rem(sp + n_sp - 1, n_sp)

    @pl.when(sp < n_sp - 1)
    def _():
        for c in halo(0, (up_to, t)):
            c.start()

    @pl.when(sp > 0)
    def _():
        for c in halo(1, (down_to, t)):
            c.start()

    def place(w, s):
        if w == 0:
            return wu.at[pl.ds(pl.multiple_of(s * depth, depth), depth), :]
        return wd.at[:, pl.ds(pl.multiple_of(s * depth, depth), depth)]

    def source(w, m):
        at = pl.ds(pl.multiple_of(m * units, units), units)
        return w_up.at[:, at] if w == 0 else w_down.at[at, :]

    flips = ((0, 1), (1, 0), (1, 1))

    def first_copy(w, k):
        fz, fx = flips[k]
        zb_, x_ = flip(zb, fz), flip(x, fx)
        return remote(source(w, zb_ * 2 + x_), place(w, sp), w_send.at[w, k], w_recv.at[w, sp],
                      (index(za, zb_, y, x_), t))

    locals_ = [pltpu.make_async_copy(source(w, me), place(w, sp), w_local.at[w]) for w in range(2)]
    for w in range(2):
        for k in range(3):
            first_copy(w, k).start()
        locals_[w].start()

    def forward(w, s, number, where):
        return remote(place(w, s), place(w, s), w_send.at[w, number], w_recv.at[w, s], where)

    def arrived(w, s):
        remote(place(w, s), place(w, s), w_send.at[w, 0], w_recv.at[w, s], (sp, u)).wait_recv()

    sent = [[], []]

    def start(w, s, where):
        number = 3 + len(sent[w])
        c = forward(w, s, number, where)
        c.start()
        sent[w].append(c)

    def spread(w):
        for k in range(4):
            if k == 0:
                locals_[w].wait()
                s = sp
            else:
                fz, fx = flips[k - 1]
                s = index(za, flip(zb, fz), y, flip(x, fx))
                arrived(w, s)
            for d in range(1, n_za):
                start(w, s, (index(lax.rem(za + d, n_za), zb, y, x), t))
            start(w, s, (index(za, zb, 1 - y, x), t))

    def relay(w):
        for k in range(4):
            fz, fx = ((0, 0),) [0] if k == 0 else flips[k - 1]
            for d in range(1, n_za):
                s = index(lax.rem(za + n_za - d, n_za), flip(zb, fz), y, flip(x, fx))
                arrived(w, s)
                start(w, s, (index(za, zb, 1 - y, x), t))

    def finish(w):
        for a in range(n_za):
            for k in range(4):
                arrived(w, index(a, k // 2, 1 - y, k % 2))

    own_k.wait()
    own_v.wait()
    own_d.wait()

    @pl.when(sp > 0)
    def _():
        for c in halo(0, (down_to, t)):
            c.wait_recv()

    @pl.when(sp == 0)
    def _():
        kx[pl.ds(0, WINDOW), :] = jnp.zeros((WINDOW, kx.shape[1]), BF16)
        vx[pl.ds(0, WINDOW), :] = jnp.zeros((WINDOW, vx.shape[1]), BF16)
        dx[:, pl.ds(0, WINDOW)] = jnp.full((8, WINDOW), -1, jnp.int32)

    @pl.when(sp < n_sp - 1)
    def _():
        for c in halo(1, (up_to, t)):
            c.wait_recv()

    @pl.when(sp == n_sp - 1)
    def _():
        end = WINDOW + rows
        kx[pl.ds(end, WINDOW), :] = jnp.zeros((WINDOW, kx.shape[1]), BF16)
        vx[pl.ds(end, WINDOW), :] = jnp.zeros((WINDOW, vx.shape[1]), BF16)
        dx[:, pl.ds(end, WINDOW)] = jnp.full((8, WINDOW), -1, jnp.int32)

    def norm_keys(b, carry):
        at = pl.ds(pl.multiple_of(b * WINDOW, WINDOW), WINDOW)
        block = kx[at, :].astype(F32)
        kn[at, :] = jnp.concatenate(
            [rms(block[:, k * head:(k + 1) * head], k_gain[...]) for k in range(kv_heads)], axis=1
        ).astype(BF16)
        return carry

    lax.fori_loop(0, kx.shape[0] // WINDOW, norm_keys, 0)

    span = 3 * WINDOW

    def attend(b, carry):
        at = pl.ds(pl.multiple_of(b * WINDOW, WINDOW), WINDOW)
        near = pl.ds(pl.multiple_of(b * WINDOW, WINDOW), span)
        far = jnp.abs(
            lax.broadcasted_iota(jnp.int32, (WINDOW, span), 1)
            - lax.broadcasted_iota(jnp.int32, (WINDOW, span), 0) - WINDOW
        )
        allowed = (far <= WINDOW) & (dx[0:1, near] == doc_col[at, :])
        mask = jnp.where(allowed, F32(0.0), F32(-1e30))
        far = far.astype(F32)
        for k in range(kv_heads):
            lanes = slice(k * head, (k + 1) * head)
            kb = kn[near, lanes]
            vb = vx[near, lanes]
            done = []
            for g in range(group):
                h = k * group + g
                qb = rms(queries[at, h * head:(h + 1) * head].astype(F32), q_gain[...]).astype(BF16)
                score = lax.dot_general(
                    qb, kb, (((1,), (1,)), ((), ())), preferred_element_type=F32
                ) * (head ** -0.5)
                score = (score - slopes[h] * far) + mask
                top = jnp.maximum(jnp.max(score, axis=-1, keepdims=True), sink[h])
                p = jnp.exp(score - top)
                denom = jnp.sum(p, axis=-1, keepdims=True) + jnp.exp(sink[h] - top)
                summed = jnp.dot(p.astype(BF16), vb, preferred_element_type=F32)
                done.append((summed / denom).astype(BF16))
                if len(done) == 2:
                    att[at, (h - 1) * head:(h + 1) * head] = jnp.concatenate(done, axis=1)
                    done = []
        return carry

    blocks = rows // WINDOW
    lax.fori_loop(0, blocks // 2, attend, 0)
    spread(0)
    lax.fori_loop(blocks // 2, blocks, attend, 0)
    spread(1)

    load_wo.wait()
    tile = 256

    def project(which, dest):
        lhs = att[pl.ds(pl.multiple_of(which * half, half), half), :]

        def step(j, carry):
            cols = pl.ds(pl.multiple_of(j * tile, tile), tile)
            dest[:, cols] = jnp.dot(lhs, wo[:, cols], preferred_element_type=F32).astype(BF16)
            return carry

        lax.fori_loop(0, width // tile, step, 0)

    project(u, other)
    swap = remote(other, other_in, misc_send.at[0], misc_recv.at[0], (sp, u))
    swap.start()
    project(t, mine)
    load_res.wait()
    swap.wait_recv()

    def middle(i, carry):
        at = pl.ds(pl.multiple_of(i * 64, 64), 64)
        both = mine[at, :].astype(F32) + other_in[at, :].astype(F32)
        value = (res[at, :].astype(F32) + both).astype(BF16)
        mid[at, :] = value
        normed[me * 2 + t, at, :] = rms(value.astype(F32), n_gain[...]).astype(BF16)
        return carry

    lax.fori_loop(0, half // 64, middle, 0)

    def token_copy(k):
        fz, fx = flips[k]
        where = (index(za, flip(zb, fz), y, flip(x, fx)), t)
        return remote(normed.at[me * 2 + t], normed.at[me * 2 + t], tok_send.at[k], tok_recv.at[k],
                      where)

    def token_arrival(k):
        fz, fx = flips[k]
        slot = (flip(zb, fz) * 2 + flip(x, fx)) * 2 + t
        return slot, remote(normed.at[slot], normed.at[slot], tok_send.at[k], tok_recv.at[k], (sp, u))

    def pair_copy(k, slot):
        return remote(normed.at[slot], normed.at[slot], pair_send.at[k], pair_recv.at[k], (sp, u))

    for k in range(3):
        token_copy(k).start()
    pair_copy(3, me * 2 + t).start()

    relay(0)
    for k in range(3):
        slot, c = token_arrival(k)
        c.wait_recv()
        pair_copy(k, slot).start()
    relay(1)
    for k in range(3):
        fz, fx = flips[k]
        pair_copy(k, (flip(zb, fz) * 2 + flip(x, fx)) * 2 + u).wait_recv()
    pair_copy(3, me * 2 + u).wait_recv()
    finish(0)
    finish(1)

    def mix(slot, put):
        lhs = normed[slot]

        def up(j, carry):
            cols = pl.ds(pl.multiple_of(j * tile, tile), tile)
            v = jnp.maximum(jnp.dot(lhs, wu[:, cols], preferred_element_type=F32), 0.0)
            act[:, cols] = (v * v).astype(BF16)
            return carry

        lax.fori_loop(0, units // tile, up, 0)
        hidden = act[...]

        def down(j, carry):
            cols = pl.ds(pl.multiple_of(j * tile, tile), tile)
            put(cols, jnp.dot(hidden, wd[:, cols], preferred_element_type=F32))
            return carry

        lax.fori_loop(0, width // tile, down, 0)

    def twin_copy(i):
        return remote(twin_out.at[i], twin_in.at[i], misc_send.at[1 + i], misc_recv.at[1 + i], (sp, u))

    def sum_copy(i, where):
        return remote(sum_out.at[i], sum_in.at[i], misc_send.at[5 + i], misc_recv.at[5 + i], where)

    order = flips[::-1] + ((0, 0),)
    sums = []
    for i, (fz, fx) in enumerate(order):
        zb_, x_ = flip(zb, fz), flip(x, fx)
        slot = (zb_ * 2 + x_) * 2

        def put_twin(cols, v, i=i):
            twin_out[i, :, cols] = v.astype(BF16)

        mix(slot + u, put_twin)
        twin_copy(i).start()

        def put_mine(cols, v):
            part[:, cols] = v

        mix(slot + t, put_mine)
        twin_copy(i).wait_recv()
        if i < 3:

            def add(r, carry, i=i):
                at = pl.ds(pl.multiple_of(r * 64, 64), 64)
                sum_out[i, at, :] = (part[at, :] + twin_in[i, at, :].astype(F32)).astype(BF16)
                return carry

            lax.fori_loop(0, half // 64, add, 0)
            c = sum_copy(i, (index(za, zb_, y, x_), t))
            c.start()
            sums.append(c)

    for i in range(3):
        sums[i].wait_recv()

    def last(r, carry):
        at = pl.ds(pl.multiple_of(r * 64, 64), 64)
        total = part[at, :] + twin_in[3, at, :].astype(F32)
        for i in range(3):
            total = total + sum_in[i, at, :].astype(F32)
        half_out[at, :] = (mid[at, :].astype(F32) + total).astype(BF16)
        return carry

    lax.fori_loop(0, half // 64, last, 0)
    final = remote(half_out, half_in, misc_send.at[8], misc_recv.at[8], (sp, u))
    final.start()
    out[pl.ds(pl.multiple_of(t * half, half), half), :] = half_out[...]
    final.wait_recv()
    out[pl.ds(pl.multiple_of(u * half, half), half), :] = half_in[...]

    final.wait_send()
    swap.wait_send()

    @pl.when(sp < n_sp - 1)
    def _():
        for c in halo(0, (up_to, t)):
            c.wait_send()

    @pl.when(sp > 0)
    def _():
        for c in halo(1, (down_to, t)):
            c.wait_send()

    for w in range(2):
        for k in range(3):
            first_copy(w, k).wait_send()
        for c in sent[w]:
            c.wait_send()
    for k in range(3):
        token_copy(k).wait_send()
    for k in range(4):
        pair_copy(k, me * 2 + t).wait_send()
    for i in range(4):
        twin_copy(i).wait_send()
    for c in sums:
        c.wait_send()


def extended(x, sides, width):
    for axis, dim in sides:
        count, length = (lax.axis_size(axis), x.shape[dim])
        up = [(i, (i + 1) % count) for i in range(count - 1)]
        down = [(j, i) for i, j in up]
        last = lax.slice_in_dim(x, length - width, length, axis=dim)
        initial = lax.slice_in_dim(x, 0, width, axis=dim)
        before = lax.ppermute(last, axis, up)
        after = lax.ppermute(initial, axis, down)
        x = jnp.concatenate([before, x, after], axis=dim)
    return x


def rms_scale(field, gain):
    wide = field.astype(jnp.float32)
    return wide * lax.rsqrt(jnp.mean(wide * wide, axis=-1, keepdims=True) + EPS) * gain


def mixer_partial(normed, w_up, w_down):
    upward = jnp.dot(
        normed, lax.all_gather(w_up, "sp", axis=0, tiled=True), preferred_element_type=jnp.float32
    )
    active = jnp.square(jax.nn.relu(upward)).astype(jnp.bfloat16)
    return jnp.dot(
        active, lax.all_gather(w_down, "sp", axis=1, tiled=True), preferred_element_type=jnp.float32
    )


def plain_shards(
    resid, queries, keys, values, documents, q_gain, k_gain, sink, w_out, n_gain, w_up, w_down
):
    rows = resid.shape[0]
    head_size = q_gain.shape[0]
    heads_here = sink.shape[0]
    kv_here = keys.shape[1] // head_size
    group = heads_here // kv_here
    qnorm = rms_scale(queries.reshape(rows, kv_here, group, head_size), q_gain).astype(jnp.bfloat16)
    knorm = rms_scale(keys.reshape(rows, kv_here, head_size), k_gain).astype(jnp.bfloat16)
    vheads = values.reshape(rows, kv_here, head_size)
    doc_here = documents.astype(jnp.bfloat16)
    near_keys, near_values, near_docs = (
        extended(knorm, (("sp", 0),), WINDOW),
        extended(vheads, (("sp", 0),), WINDOW),
        extended(doc_here, (("sp", 0),), WINDOW),
    )
    offset = lax.axis_index("sp") * rows
    total = rows * lax.axis_size("sp")
    query_pos = offset + jnp.arange(rows, dtype=jnp.int32)
    key_pos = offset - WINDOW + jnp.arange(rows + 2 * WINDOW, dtype=jnp.int32)
    distance = key_pos[None, :] - query_pos[:, None]
    allowed = (jnp.abs(distance) <= WINDOW) & (key_pos[None, :] >= 0) & (key_pos[None, :] < total)
    allowed = allowed & (near_docs[None, :] == doc_here[:, None])
    heads_all = heads_here * lax.axis_size("tp")
    first_head = (lax.axis_index("tp") * heads_here).astype(jnp.float32)
    slopes = jnp.exp2(
        -8.0 * (first_head + jnp.arange(heads_here, dtype=jnp.float32) + 1.0) / heads_all
    )
    slopes = slopes.reshape(kv_here, group)
    sink_f = sink.reshape(kv_here, group)
    scores = jnp.einsum(
        "rkgd,skd->kgrs", qnorm, near_keys, preferred_element_type=jnp.float32
    ) * head_size ** (-0.5)
    scores = scores - slopes[:, :, None, None] * jnp.abs(distance).astype(jnp.float32)[None, None]
    scores = jnp.where(allowed[None, None], scores, jnp.float32(-1e30))
    highest = jnp.maximum(jnp.max(scores, axis=-1), sink_f[:, :, None])
    weights = jnp.exp(scores - highest[..., None])
    denom = jnp.sum(weights, axis=-1) + jnp.exp(sink_f[:, :, None] - highest)
    summed = jnp.einsum(
        "kgrs,skd->rkgd",
        weights.astype(jnp.bfloat16),
        near_values,
        preferred_element_type=jnp.float32,
    )
    attended = (
        (summed / denom.transpose(2, 0, 1)[..., None])
        .astype(jnp.bfloat16)
        .reshape(rows, heads_here * head_size)
    )
    head_mix = lax.psum(
        jnp.dot(attended, w_out, preferred_element_type=jnp.float32).astype(jnp.bfloat16), "tp"
    ).astype(jnp.float32)
    middle = (resid.astype(jnp.float32) + head_mix).astype(jnp.bfloat16)
    normed = rms_scale(middle, n_gain).astype(jnp.bfloat16)
    partial_sum = mixer_partial(normed, w_up, w_down)
    unit_mix = lax.psum(partial_sum.astype(jnp.bfloat16), "tp").astype(jnp.float32)
    return (middle.astype(jnp.float32) + unit_mix).astype(jnp.bfloat16)


def fused_shards(
    resid, queries, keys, values, documents, q_gain, k_gain, sink, w_out, n_gain, w_up, w_down
):
    rows, width = resid.shape
    half = rows // 2
    n_sp = lax.axis_size("sp")
    head = q_gain.shape[0]
    heads = sink.shape[0]
    kv_heads = keys.shape[1] // head
    units = w_up.shape[1] // MEMBERS
    n_za = n_sp // 8
    first = (lax.axis_index("tp") * heads).astype(F32)
    slopes = jnp.exp2(
        -8.0 * (first + jnp.arange(heads, dtype=F32) + 1.0) / (heads * lax.axis_size("tp"))
    )
    vmem = pl.BlockSpec(memory_space=pltpu.VMEM)
    smem = pl.BlockSpec(memory_space=pltpu.SMEM)
    hbm = pl.BlockSpec(memory_space=pl.ANY)
    sends = 3 + 4 * n_za + 4 * (n_za - 1)
    dma = pltpu.SemaphoreType.DMA
    return pl.pallas_call(
        functools.partial(kernel, n_sp, head, heads, kv_heads),
        out_shape=jax.ShapeDtypeStruct((rows, width), BF16),
        in_specs=[hbm, vmem, vmem, vmem, vmem, vmem, vmem, vmem, smem, smem, hbm, vmem, hbm, hbm],
        out_specs=vmem,
        scratch_shapes=[
            pltpu.VMEM((rows + 2 * WINDOW, keys.shape[1]), BF16),
            pltpu.VMEM((rows + 2 * WINDOW, keys.shape[1]), BF16),
            pltpu.VMEM((8, rows + 2 * WINDOW), jnp.int32),
            pltpu.VMEM((rows + 2 * WINDOW, keys.shape[1]), BF16),
            pltpu.VMEM((rows, heads * head), BF16),
            pltpu.VMEM(w_out.shape, BF16),
            pltpu.VMEM((half, width), BF16),
            pltpu.VMEM((half, width), BF16),
            pltpu.VMEM((half, width), BF16),
            pltpu.VMEM((half, width), BF16),
            pltpu.VMEM((half, width), BF16),
            pltpu.VMEM((2 * MEMBERS, half, width), BF16),
            pltpu.VMEM((width, units), BF16),
            pltpu.VMEM((units, width), BF16),
            pltpu.VMEM((half, units), BF16),
            pltpu.VMEM((half, width), F32),
            pltpu.VMEM((4, half, width), BF16),
            pltpu.VMEM((4, half, width), BF16),
            pltpu.VMEM((3, half, width), BF16),
            pltpu.VMEM((3, half, width), BF16),
            pltpu.VMEM((half, width), BF16),
            pltpu.VMEM((half, width), BF16),
            dma((2, 3)),
            dma((2, 3)),
            dma((2, sends)),
            dma((2, n_sp)),
            dma((2,)),
            dma((5,)),
            dma((3,)),
            dma((3,)),
            dma((4,)),
            dma((4,)),
            dma((9,)),
            dma((9,)),
        ],
        compiler_params=pltpu.CompilerParams(
            has_side_effects=True, vmem_limit_bytes=62 * 1024 * 1024
        ),
        name="layer",
    )(
        resid,
        queries,
        keys,
        values,
        documents[:, None],
        jnp.broadcast_to(documents[None, :], (8, rows)),
        q_gain[None, :],
        k_gain[None, :],
        slopes,
        sink,
        w_out,
        n_gain[None, :],
        w_up,
        w_down,
    )


def solution(mesh):
    placed = (
        P("sp", None),
        P("sp", "tp"),
        P("sp", "tp"),
        P("sp", "tp"),
        P("sp"),
        P(),
        P(),
        P("tp"),
        P("tp", None),
        P(),
        P("sp", "tp"),
        P("tp", "sp"),
    )
    sizes = dict(mesh.shape)

    def shards(*args):
        columns = args[11].shape[1]
        fits = sizes["tp"] == 2 and sizes["sp"] % 8 == 0 and columns % 128 == 0
        return (fused_shards if fits else plain_shards)(*args)

    return jax.shard_map(
        shards, mesh=mesh, in_specs=placed, out_specs=P("sp", None), check_vma=False
    )
```

```python
import functools

import jax
import jax.numpy as jnp
from jax import lax
from jax.experimental import pallas as pl
from jax.experimental.pallas import tpu as pltpu
from jax.sharding import PartitionSpec as P

WINDOW = 128
EPS = 1e-06
MEMBERS = 4
F32 = jnp.float32
BF16 = jnp.bfloat16
MESH = pl.DeviceIdType.MESH


def rms(wide, gain):
    return wide * lax.rsqrt(jnp.mean(wide * wide, axis=-1, keepdims=True) + EPS) * gain


def kernel(
    n_sp,
    head,
    heads,
    kv_heads,
    resid,
    queries,
    keys,
    values,
    doc_col,
    doc_row,
    q_gain,
    k_gain,
    slopes,
    sink,
    w_out,
    n_gain,
    w_up,
    w_down,
    out,
    kx,
    vx,
    dx,
    kn,
    att,
    wo,
    res,
    mine,
    other,
    other_in,
    mid,
    normed,
    wu,
    wd,
    act,
    part,
    twin_out,
    twin_in,
    sum_out,
    sum_in,
    half_out,
    half_in,
    halo_send,
    halo_recv,
    w_send,
    w_recv,
    w_local,
    loc_sem,
    tok_send,
    tok_recv,
    pair_send,
    pair_recv,
    swap_send,
    swap_recv,
    misc_send,
    misc_recv,
):
    rows = queries.shape[0]
    half = rows // 2
    depth = w_up.shape[0]
    units = wu.shape[1]
    width = wd.shape[1]
    group = heads // kv_heads
    n_za = n_sp // 8

    sp = lax.axis_index("sp")
    t = lax.axis_index("tp")
    u = 1 - t
    x = sp % 2
    y = (sp // 2) % 2
    zb = (sp // 4) % 2
    za = sp // 8
    me = zb * 2 + x

    def index(za_, zb_, y_, x_):
        return za_ * 8 + zb_ * 4 + y_ * 2 + x_

    def flip(v, by):
        return 1 - v if by else v

    def remote(src, dst, send, recv, where):
        return pltpu.make_async_remote_copy(
            src_ref=src, dst_ref=dst, send_sem=send, recv_sem=recv,
            device_id=where, device_id_type=MESH,
        )

    up_to = lax.rem(sp + 1, n_sp)
    down_to = lax.rem(sp + n_sp - 1, n_sp)
    partners = [(sp, u), (up_to, t), (down_to, t), (index(za, zb, 1 - y, x), t)]
    partners += [(index(za, flip(zb, fz), y, flip(x, fx)), t) for fz, fx in ((0, 1), (1, 0), (1, 1))]
    partners += [(index(lax.rem(za + d, n_za), zb, y, x), t) for d in range(1, n_za)]
    with jax.named_scope("barrier"):
        greeting = pltpu.get_barrier_semaphore()
        for where in partners:
            pl.semaphore_signal(greeting, inc=1, device_id=where, device_id_type=MESH)
        pl.semaphore_wait(greeting, len(partners))

    load_wo = pltpu.make_async_copy(w_out, wo, loc_sem.at[0])
    load_wo.start()
    load_res = pltpu.make_async_copy(resid.at[pl.ds(t * half, half), :], res, loc_sem.at[1])
    load_res.start()
    own_k = pltpu.make_async_copy(keys, kx.at[pl.ds(WINDOW, rows), :], loc_sem.at[2])
    own_v = pltpu.make_async_copy(values, vx.at[pl.ds(WINDOW, rows), :], loc_sem.at[3])
    own_d = pltpu.make_async_copy(doc_row, dx.at[:, pl.ds(WINDOW, rows)], loc_sem.at[4])
    own_k.start()
    own_v.start()
    own_d.start()

    def halo(side, where):
        src = rows - WINDOW if side == 0 else 0
        dst = 0 if side == 0 else WINDOW + rows
        return [
            remote(keys.at[pl.ds(src, WINDOW), :], kx.at[pl.ds(dst, WINDOW), :],
                   halo_send.at[side, 0], halo_recv.at[side, 0], where),
            remote(values.at[pl.ds(src, WINDOW), :], vx.at[pl.ds(dst, WINDOW), :],
                   halo_send.at[side, 1], halo_recv.at[side, 1], where),
            remote(doc_row.at[:, pl.ds(src, WINDOW)], dx.at[:, pl.ds(dst, WINDOW)],
                   halo_send.at[side, 2], halo_recv.at[side, 2], where),
        ]

    @pl.when(sp < n_sp - 1)
    def _():
        for c in halo(0, (up_to, t)):
            c.start()

    @pl.when(sp > 0)
    def _():
        for c in halo(1, (down_to, t)):
            c.start()

    def place(w, s):
        if w == 0:
            return wu.at[pl.ds(pl.multiple_of(s * depth, depth), depth), :]
        return wd.at[:, pl.ds(pl.multiple_of(s * depth, depth), depth)]

    def source(w, m):
        at = pl.ds(pl.multiple_of(m * units, units), units)
        return w_up.at[:, at] if w == 0 else w_down.at[at, :]

    flips = ((0, 1), (1, 0), (1, 1))

    def first_copy(w, k):
        fz, fx = flips[k]
        zb_, x_ = flip(zb, fz), flip(x, fx)
        return remote(source(w, zb_ * 2 + x_), place(w, sp), w_send.at[w, k], w_recv.at[w, sp],
                      (index(za, zb_, y, x_), t))

    locals_ = [pltpu.make_async_copy(source(w, me), place(w, sp), w_local.at[w]) for w in range(2)]
    def arrived(w, s):
        remote(place(w, s), place(w, s), w_send.at[w, 0], w_recv.at[w, s], (sp, u)).wait_recv()

    sent = [[], []]

    def start(w, s, where, src=None):
        c = remote(place(w, s) if src is None else src, place(w, s), w_send.at[w, 3 + len(sent[w])],
                   w_recv.at[w, s], where)
        c.start()
        sent[w].append(c)

    def onward(w, s, src=None):
        for d in range(1, n_za):
            start(w, s, (index(lax.rem(za + d, n_za), zb, y, x), t), src)
        start(w, s, (index(za, zb, 1 - y, x), t), src)

    def exchange(w):
        for k in range(3):
            first_copy(w, k).start()
        locals_[w].start()

    def spread_own(w):
        onward(w, sp, source(w, me))

    def spread(w):
        with jax.named_scope(f"spread#w={w}"):
            for fz, fx in flips:
                s = index(za, flip(zb, fz), y, flip(x, fx))
                arrived(w, s)
                onward(w, s)

    def relay(w, k):
        fz, fx = ((0, 0),) [0] if k == 0 else flips[k - 1]
        with jax.named_scope(f"relay#w={w}#k={k}"):
            for d in range(1, n_za):
                s = index(lax.rem(za + n_za - d, n_za), flip(zb, fz), y, flip(x, fx))
                arrived(w, s)
                start(w, s, (index(za, zb, 1 - y, x), t))

    def finish(w):
        with jax.named_scope(f"finish#w={w}"):
            locals_[w].wait()
            for a in range(n_za):
                for k in range(4):
                    arrived(w, index(a, k // 2, 1 - y, k % 2))

    exchange(0)
    spread_own(0)

    with jax.named_scope("own_wait"):
        own_k.wait()
        own_v.wait()
        own_d.wait()

    @pl.when(sp > 0)
    def _():
        for c in halo(0, (down_to, t)):
            c.wait_recv()

    @pl.when(sp == 0)
    def _():
        kx[pl.ds(0, WINDOW), :] = jnp.zeros((WINDOW, kx.shape[1]), BF16)
        vx[pl.ds(0, WINDOW), :] = jnp.zeros((WINDOW, vx.shape[1]), BF16)
        dx[:, pl.ds(0, WINDOW)] = jnp.full((8, WINDOW), -1, jnp.int32)

    @pl.when(sp < n_sp - 1)
    def _():
        for c in halo(1, (up_to, t)):
            c.wait_recv()

    @pl.when(sp == n_sp - 1)
    def _():
        end = WINDOW + rows
        kx[pl.ds(end, WINDOW), :] = jnp.zeros((WINDOW, kx.shape[1]), BF16)
        vx[pl.ds(end, WINDOW), :] = jnp.zeros((WINDOW, vx.shape[1]), BF16)
        dx[:, pl.ds(end, WINDOW)] = jnp.full((8, WINDOW), -1, jnp.int32)

    def norm_keys(b, carry):
        at = pl.ds(pl.multiple_of(b * WINDOW, WINDOW), WINDOW)
        block = kx[at, :].astype(F32)
        kn[at, :] = jnp.concatenate(
            [rms(block[:, k * head:(k + 1) * head], k_gain[...]) for k in range(kv_heads)], axis=1
        ).astype(BF16)
        return carry

    exchange(1)
    with jax.named_scope("norm_keys"):
        lax.fori_loop(0, kx.shape[0] // WINDOW, norm_keys, 0)

    span = 3 * WINDOW

    def attend(b, carry):
        at = pl.ds(pl.multiple_of(b * WINDOW, WINDOW), WINDOW)
        near = pl.ds(pl.multiple_of(b * WINDOW, WINDOW), span)
        far = jnp.abs(
            lax.broadcasted_iota(jnp.int32, (WINDOW, span), 1)
            - lax.broadcasted_iota(jnp.int32, (WINDOW, span), 0) - WINDOW
        )
        allowed = (far <= WINDOW) & (dx[0:1, near] == doc_col[at, :])
        mask = jnp.where(allowed, F32(0.0), F32(-1e30))
        far = far.astype(F32)
        for k in range(kv_heads):
            lanes = slice(k * head, (k + 1) * head)
            kb = kn[near, lanes]
            vb = vx[near, lanes]
            done = []
            for g in range(group):
                h = k * group + g
                qb = rms(queries[at, h * head:(h + 1) * head].astype(F32), q_gain[...]).astype(BF16)
                score = lax.dot_general(
                    qb, kb, (((1,), (1,)), ((), ())), preferred_element_type=F32
                ) * (head ** -0.5)
                score = (score - slopes[h] * far) + mask
                top = jnp.maximum(jnp.max(score, axis=-1, keepdims=True), sink[h])
                p = jnp.exp(score - top)
                denom = jnp.sum(p, axis=-1, keepdims=True) + jnp.exp(sink[h] - top)
                summed = jnp.dot(p.astype(BF16), vb, preferred_element_type=F32)
                done.append((summed / denom).astype(BF16))
                if len(done) == 2:
                    att[at, (h - 1) * head:(h + 1) * head] = jnp.concatenate(done, axis=1)
                    done = []
        return carry

    tile = 256
    rounds = half // WINDOW
    swaps = []

    def project(row, dest):
        lhs = att[pl.ds(pl.multiple_of(row, WINDOW), WINDOW), :]

        def step(j, carry):
            cols = pl.ds(pl.multiple_of(j * tile, tile), tile)
            dest[:, cols] = jnp.dot(lhs, wo[:, cols], preferred_element_type=F32).astype(BF16)
            return carry

        lax.fori_loop(0, width // tile, step, 0)

    def token_rows(slot, r):
        return normed.at[pl.ds(pl.multiple_of(slot * half + r * WINDOW, WINDOW), WINDOW), :]

    def token_copy(k, r):
        fz, fx = flips[k]
        where = (index(za, flip(zb, fz), y, flip(x, fx)), t)
        rows_ = token_rows(me * 2 + t, r)
        return remote(rows_, rows_, tok_send.at[k, r], tok_recv.at[k, r], where)

    def member(k):
        if k == 3:
            return me
        fz, fx = flips[k]
        return flip(zb, fz) * 2 + flip(x, fx)

    def pair_copy(k, core, r):
        rows_ = token_rows(member(k) * 2 + core, r)
        return remote(rows_, rows_, pair_send.at[k, r], pair_recv.at[k, r], (sp, u))

    def token_pass(k, r):
        with jax.named_scope(f"token#k={k}#r={r}"):
            rows_ = token_rows(member(k) * 2 + t, r)
            remote(rows_, rows_, tok_send.at[k, r], tok_recv.at[k, r], (sp, u)).wait_recv()
            if k == 1:
                token_relay(r).start()
            pair_copy(k, t, r).start()

    def token_relay(r):
        rows_ = token_rows(member(1) * 2 + t, r)
        return remote(rows_, rows_, tok_send.at[2, r], tok_recv.at[2, r],
                      (index(za, zb, y, 1 - x), t))

    def one_round(r):
        with jax.named_scope("project"):
            project(u * half + r * WINDOW, other.at[r])
            swap = remote(other.at[r], other_in.at[r], swap_send.at[r], swap_recv.at[r], (sp, u))
            swap.start()
            swaps.append(swap)
            project(t * half + r * WINDOW, mine.at[r])
        with jax.named_scope("swap_wait"):
            swap.wait_recv()

        def middle(i, carry):
            at = pl.ds(pl.multiple_of(i * 64, 64), 64)
            here = pl.ds(pl.multiple_of(r * WINDOW + i * 64, 64), 64)
            both = mine[r, at, :].astype(F32) + other_in[r, at, :].astype(F32)
            value = (res[here, :].astype(F32) + both).astype(BF16)
            mid[here, :] = value
            row = pl.multiple_of((me * 2 + t) * half + r * WINDOW + i * 64, 64)
            normed[pl.ds(row, 64), :] = rms(value.astype(F32), n_gain[...]).astype(BF16)
            return carry

        lax.fori_loop(0, WINDOW // 64, middle, 0)
        for k in (1, 0):
            token_copy(k, r).start()
        pair_copy(3, t, r).start()

    def attend_pair(r, between):
        with jax.named_scope("attend"):
            lax.fori_loop(r, r + 1, attend, 0)
        between()
        with jax.named_scope("attend"):
            lax.fori_loop(r + rounds, r + rounds + 1, attend, 0)

    for r in range(rounds):
        if r == 0:
            attend_pair(r, lambda: spread(0))
            spread_own(1)
            load_wo.wait()
            load_res.wait()
        elif r == 1:
            attend_pair(r, lambda: relay(0, 0))
            relay(0, 1)
        else:
            attend_pair(r, lambda: None)
        one_round(r)

    def up(m):
        row = pl.multiple_of(m * rows, rows)

        def step(j, carry):
            cols = pl.ds(pl.multiple_of(j * tile, tile), tile)
            v = jnp.dot(normed[pl.ds(row, rows), :], wu[:, cols], preferred_element_type=F32)
            v = jnp.maximum(v, 0.0)
            act[pl.ds(row, rows), cols] = (v * v).astype(BF16)
            return carry

        with jax.named_scope("up"):
            lax.fori_loop(0, units // tile, step, 0)

    def pair_wait(k):
        with jax.named_scope("pair_wait"):
            for r in range(rounds):
                pair_copy(k, u, r).wait_recv()

    spread(1)
    if rounds < 2:
        relay(0, 0)
        relay(0, 1)
    for r in range(rounds - 1):
        token_pass(1, r)
    relay(0, 2)
    relay(0, 3)
    token_pass(1, rounds - 1)
    relay(1, 0)
    finish(0)
    pair_wait(3)
    up(me)
    for r in range(rounds):
        token_pass(0, r)
    relay(1, 1)
    pair_wait(0)
    up(member(0))
    for r in range(rounds):
        token_pass(2, r)
    relay(1, 2)
    relay(1, 3)
    for k in (1, 2):
        pair_wait(k)
        up(member(k))
    finish(1)

    def twin_copy(i):
        return remote(twin_out.at[i], twin_in.at[i], misc_send.at[1 + i], misc_recv.at[1 + i], (sp, u))

    def sum_copy(i, where):
        return remote(sum_out.at[i], sum_in.at[i], misc_send.at[5 + i], misc_recv.at[5 + i], where)

    order = flips[::-1] + ((0, 0),)
    sums = []
    for i, (fz, fx) in enumerate(order):
        zb_, x_ = flip(zb, fz), flip(x, fx)
        row = pl.multiple_of((zb_ * 2 + x_) * rows, rows)

        def down(j, carry, i=i, row=row):
            cols = pl.ds(pl.multiple_of(j * tile, tile), tile)
            v = jnp.dot(act[pl.ds(row, rows), :], wd[:, cols], preferred_element_type=F32)
            low, high = v[:half], v[half:]
            twin_out[i, :, cols] = jnp.where(t == 0, high, low).astype(BF16)
            part[:, cols] = jnp.where(t == 0, low, high)
            return carry

        with jax.named_scope("down"):
            lax.fori_loop(0, width // tile, down, 0)
        twin_copy(i).start()
        with jax.named_scope("twin_wait"):
            twin_copy(i).wait_recv()
        if i < 3:

            def add(r, carry, i=i):
                at = pl.ds(pl.multiple_of(r * 64, 64), 64)
                sum_out[i, at, :] = (part[at, :] + twin_in[i, at, :].astype(F32)).astype(BF16)
                return carry

            lax.fori_loop(0, half // 64, add, 0)
            c = sum_copy(i, (index(za, zb_, y, x_), t))
            c.start()
            sums.append(c)

    with jax.named_scope("sum_wait"):
        for i in range(3):
            sums[i].wait_recv()

    def last(r, carry):
        at = pl.ds(pl.multiple_of(r * 64, 64), 64)
        total = part[at, :] + twin_in[3, at, :].astype(F32)
        for i in range(3):
            total = total + sum_in[i, at, :].astype(F32)
        half_out[at, :] = (mid[at, :].astype(F32) + total).astype(BF16)
        return carry

    lax.fori_loop(0, half // 64, last, 0)
    final = remote(half_out, half_in, misc_send.at[0], misc_recv.at[0], (sp, u))
    final.start()
    out[pl.ds(pl.multiple_of(t * half, half), half), :] = half_out[...]
    with jax.named_scope("final_wait"):
        final.wait_recv()
    out[pl.ds(pl.multiple_of(u * half, half), half), :] = half_in[...]

    final.wait_send()
    for swap in swaps:
        swap.wait_send()

    @pl.when(sp < n_sp - 1)
    def _():
        for c in halo(0, (up_to, t)):
            c.wait_send()

    @pl.when(sp > 0)
    def _():
        for c in halo(1, (down_to, t)):
            c.wait_send()

    for w in range(2):
        for k in range(3):
            first_copy(w, k).wait_send()
        for c in sent[w]:
            c.wait_send()
    for r in range(rounds):
        for k in range(2):
            token_copy(k, r).wait_send()
        token_relay(r).wait_send()
        for k in range(4):
            pair_copy(k, t, r).wait_send()
    for i in range(4):
        twin_copy(i).wait_send()
    for c in sums:
        c.wait_send()


def extended(x, sides, width):
    for axis, dim in sides:
        count, length = (lax.axis_size(axis), x.shape[dim])
        up = [(i, (i + 1) % count) for i in range(count - 1)]
        down = [(j, i) for i, j in up]
        last = lax.slice_in_dim(x, length - width, length, axis=dim)
        initial = lax.slice_in_dim(x, 0, width, axis=dim)
        before = lax.ppermute(last, axis, up)
        after = lax.ppermute(initial, axis, down)
        x = jnp.concatenate([before, x, after], axis=dim)
    return x


def rms_scale(field, gain):
    wide = field.astype(jnp.float32)
    return wide * lax.rsqrt(jnp.mean(wide * wide, axis=-1, keepdims=True) + EPS) * gain


def mixer_partial(normed, w_up, w_down):
    upward = jnp.dot(
        normed, lax.all_gather(w_up, "sp", axis=0, tiled=True), preferred_element_type=jnp.float32
    )
    active = jnp.square(jax.nn.relu(upward)).astype(jnp.bfloat16)
    return jnp.dot(
        active, lax.all_gather(w_down, "sp", axis=1, tiled=True), preferred_element_type=jnp.float32
    )


def plain_shards(
    resid, queries, keys, values, documents, q_gain, k_gain, sink, w_out, n_gain, w_up, w_down
):
    rows = resid.shape[0]
    head_size = q_gain.shape[0]
    heads_here = sink.shape[0]
    kv_here = keys.shape[1] // head_size
    group = heads_here // kv_here
    qnorm = rms_scale(queries.reshape(rows, kv_here, group, head_size), q_gain).astype(jnp.bfloat16)
    knorm = rms_scale(keys.reshape(rows, kv_here, head_size), k_gain).astype(jnp.bfloat16)
    vheads = values.reshape(rows, kv_here, head_size)
    doc_here = documents.astype(jnp.bfloat16)
    near_keys, near_values, near_docs = (
        extended(knorm, (("sp", 0),), WINDOW),
        extended(vheads, (("sp", 0),), WINDOW),
        extended(doc_here, (("sp", 0),), WINDOW),
    )
    offset = lax.axis_index("sp") * rows
    total = rows * lax.axis_size("sp")
    query_pos = offset + jnp.arange(rows, dtype=jnp.int32)
    key_pos = offset - WINDOW + jnp.arange(rows + 2 * WINDOW, dtype=jnp.int32)
    distance = key_pos[None, :] - query_pos[:, None]
    allowed = (jnp.abs(distance) <= WINDOW) & (key_pos[None, :] >= 0) & (key_pos[None, :] < total)
    allowed = allowed & (near_docs[None, :] == doc_here[:, None])
    heads_all = heads_here * lax.axis_size("tp")
    first_head = (lax.axis_index("tp") * heads_here).astype(jnp.float32)
    slopes = jnp.exp2(
        -8.0 * (first_head + jnp.arange(heads_here, dtype=jnp.float32) + 1.0) / heads_all
    )
    slopes = slopes.reshape(kv_here, group)
    sink_f = sink.reshape(kv_here, group)
    scores = jnp.einsum(
        "rkgd,skd->kgrs", qnorm, near_keys, preferred_element_type=jnp.float32
    ) * head_size ** (-0.5)
    scores = scores - slopes[:, :, None, None] * jnp.abs(distance).astype(jnp.float32)[None, None]
    scores = jnp.where(allowed[None, None], scores, jnp.float32(-1e30))
    highest = jnp.maximum(jnp.max(scores, axis=-1), sink_f[:, :, None])
    weights = jnp.exp(scores - highest[..., None])
    denom = jnp.sum(weights, axis=-1) + jnp.exp(sink_f[:, :, None] - highest)
    summed = jnp.einsum(
        "kgrs,skd->rkgd",
        weights.astype(jnp.bfloat16),
        near_values,
        preferred_element_type=jnp.float32,
    )
    attended = (
        (summed / denom.transpose(2, 0, 1)[..., None])
        .astype(jnp.bfloat16)
        .reshape(rows, heads_here * head_size)
    )
    head_mix = lax.psum(
        jnp.dot(attended, w_out, preferred_element_type=jnp.float32).astype(jnp.bfloat16), "tp"
    ).astype(jnp.float32)
    middle = (resid.astype(jnp.float32) + head_mix).astype(jnp.bfloat16)
    normed = rms_scale(middle, n_gain).astype(jnp.bfloat16)
    partial_sum = mixer_partial(normed, w_up, w_down)
    unit_mix = lax.psum(partial_sum.astype(jnp.bfloat16), "tp").astype(jnp.float32)
    return (middle.astype(jnp.float32) + unit_mix).astype(jnp.bfloat16)


def fused_shards(
    resid, queries, keys, values, documents, q_gain, k_gain, sink, w_out, n_gain, w_up, w_down
):
    rows, width = resid.shape
    half = rows // 2
    n_sp = lax.axis_size("sp")
    head = q_gain.shape[0]
    heads = sink.shape[0]
    kv_heads = keys.shape[1] // head
    units = w_up.shape[1] // MEMBERS
    n_za = n_sp // 8
    rounds = half // WINDOW
    first = (lax.axis_index("tp") * heads).astype(F32)
    slopes = jnp.exp2(
        -8.0 * (first + jnp.arange(heads, dtype=F32) + 1.0) / (heads * lax.axis_size("tp"))
    )
    vmem = pl.BlockSpec(memory_space=pltpu.VMEM)
    smem = pl.BlockSpec(memory_space=pltpu.SMEM)
    hbm = pl.BlockSpec(memory_space=pl.ANY)
    sends = 3 + 4 * n_za + 4 * (n_za - 1)
    dma = pltpu.SemaphoreType.DMA
    return pl.pallas_call(
        functools.partial(kernel, n_sp, head, heads, kv_heads),
        out_shape=jax.ShapeDtypeStruct((rows, width), BF16),
        in_specs=[hbm, vmem, vmem, vmem, vmem, vmem, vmem, vmem, smem, smem, hbm, vmem, hbm, hbm],
        out_specs=vmem,
        scratch_shapes=[
            pltpu.VMEM((rows + 2 * WINDOW, keys.shape[1]), BF16),
            pltpu.VMEM((rows + 2 * WINDOW, keys.shape[1]), BF16),
            pltpu.VMEM((8, rows + 2 * WINDOW), jnp.int32),
            pltpu.VMEM((rows + 2 * WINDOW, keys.shape[1]), BF16),
            pltpu.VMEM((rows, heads * head), BF16),
            pltpu.VMEM(w_out.shape, BF16),
            pltpu.VMEM((half, width), BF16),
            pltpu.VMEM((rounds, WINDOW, width), BF16),
            pltpu.VMEM((rounds, WINDOW, width), BF16),
            pltpu.VMEM((rounds, WINDOW, width), BF16),
            pltpu.VMEM((half, width), BF16),
            pltpu.VMEM((MEMBERS * rows, width), BF16),
            pltpu.VMEM((width, units), BF16),
            pltpu.VMEM((units, width), BF16),
            pltpu.VMEM((MEMBERS * rows, units), BF16),
            pltpu.VMEM((half, width), F32),
            pltpu.VMEM((4, half, width), BF16),
            pltpu.VMEM((4, half, width), BF16),
            pltpu.VMEM((3, half, width), BF16),
            pltpu.VMEM((3, half, width), BF16),
            pltpu.VMEM((half, width), BF16),
            pltpu.VMEM((half, width), BF16),
            dma((2, 3)),
            dma((2, 3)),
            dma((2, sends)),
            dma((2, n_sp)),
            dma((2,)),
            dma((5,)),
            dma((3, rounds)),
            dma((3, rounds)),
            dma((4, rounds)),
            dma((4, rounds)),
            dma((rounds,)),
            dma((rounds,)),
            dma((8,)),
            dma((8,)),
        ],
        compiler_params=pltpu.CompilerParams(
            collective_id=0, has_side_effects=True, vmem_limit_bytes=62 * 1024 * 1024
        ),
        name="layer",
    )(
        resid,
        queries,
        keys,
        values,
        documents[:, None],
        jnp.broadcast_to(documents[None, :], (8, rows)),
        q_gain[None, :],
        k_gain[None, :],
        slopes,
        sink,
        w_out,
        n_gain[None, :],
        w_up,
        w_down,
    )


def solution(mesh):
    placed = (
        P("sp", None),
        P("sp", "tp"),
        P("sp", "tp"),
        P("sp", "tp"),
        P("sp"),
        P(),
        P(),
        P("tp"),
        P("tp", None),
        P(),
        P("sp", "tp"),
        P("tp", "sp"),
    )
    sizes = dict(mesh.shape)

    def shards(*args):
        columns = args[11].shape[1]
        fits = sizes["tp"] == 2 and sizes["sp"] % 8 == 0 and columns % 128 == 0
        return (fused_shards if fits else plain_shards)(*args)

    return jax.shard_map(
        shards, mesh=mesh, in_specs=placed, out_specs=P("sp", None), check_vma=False
    )
```
